32 devices in a mesh: sp: 16 (over z, y, x), tp: 2 (over core).
Axes of the slice: x: 2, y: 2, z: 4, core: 2. Of those that a mesh axis runs over, the one named last changes fastest.
Arguments:
- latent: bfloat16 [4096, 256], P('sp'), may hold values from -6 to 6
- rotary_key: bfloat16 [4096, 64], P('sp'), may hold values from -7 to 7
- doc_ids: int32 [4096], P('sp'), may hold values from 0 to 7, never falling along the last dimension, each value on 1 to 1024 neighbouring positions
- queries_content: bfloat16 [4096, 1024], P('sp', 'tp'), may hold values from -6 to 6
- queries_rotary: bfloat16 [4096, 512], P('sp', 'tp'), may hold values from -400 to 400
- w_key_up: bfloat16 [256, 1024], replicated, may hold values from -0.375 to 0.375
- w_value_up: bfloat16 [256, 1024], replicated, may hold values from -0.375 to 0.375
- w_out: bfloat16 [1024, 2048], P('tp'), may hold values from -1.5 to 1.5
- residual: bfloat16 [4096, 2048], P(('sp', 'tp')), may hold values from -4 to 4
- norm_gain: float32 [2048], replicated, may hold values from 0.1 to 1.9
- routes: int32 [4096, 2], P(('sp', 'tp')), may hold values from 0 to 15, all different within a row; in each aligned block of 128 rows (0 to 127, 128 to 255, ...) at most 32 rows name the same one
- route_weights: float32 [4096, 2], P(('sp', 'tp')), may hold values from 0.1 to 1
- w_gate: bfloat16 [16, 2048, 3584], P('sp', None, 'tp'), may hold values from -0.125 to 0.125
- w_up: bfloat16 [16, 2048, 3584], P('sp', None, 'tp'), may hold values from -0.125 to 0.125
- w_down: bfloat16 [16, 3584, 2048], P('sp', 'tp'), may hold values from -0.09375 to 0.09375
- out_gain: float32 [2048], replicated, may hold values from 0.1 to 1.9
Outputs:
- mixed: bfloat16 [4096, 2048], P(('sp', 'tp'))
The draws below stay inside these ranges and needn't reach their ends.
Inputs may be any that keep to these rules, and one draw needn't show every extreme that they name: `doc_ids`: document numbers never fall along positions; each document holds 1 to 1024 positions, and one holds exactly 1024. `routes`: each row names 2 different experts; among the rows of one device (aligned blocks of 128 rows) no expert is named more than 32 times, and in some blocks one expert is named exactly 32 times.
All inputs are finite; a program needn't handle non-finite values.
Results may differ from the reference program's by a relative error of at most 0.014.
Values may be sent and summed in bfloat16 or wider, within the bound.
A program may use at most 128 MiB of HBM per device.

```python
import math
import jax
import jax.numpy as jnp
import numpy as np
from jax import lax

D = 2048
HEADS = 8
DK = 128
DR = 64
DV = 128
RANK = 256
FF = 3584
TOPK = 2
REACH = 4
TOK_DEV = 256
TOKENS = 4096
ROWS = 128
EXPERTS = 16
CAP = 32
DOCS = 8
DOC_MOST = 1024
N_SP = 16
N_TP = 2


def rotary_base(key):
    rotary_draw = jnp.clip(jax.random.normal(jax.random.fold_in(key, 7), (TOKENS, DR), jnp.float32), -4.5, 4.5)
    return rotary_draw


def draw_rotary_key(key, part):
    return rotary_base(key).astype(jnp.bfloat16)


def draw_queries_rotary(key, part):
    drawn = jax.random.normal(jax.random.fold_in(key, 8), (TOKENS, HEADS, DR), jnp.float32)
    return drawn.reshape(TOKENS, HEADS * DR).astype(jnp.bfloat16)


def levels(stream_key, shape, cuts, smallest, high):
    gain = 1.0
    for dim, shards_of in cuts:
        steps = jax.random.uniform(jax.random.fold_in(jax.random.fold_in(stream_key, 6), dim), (shards_of,), jnp.float32, smallest / len(cuts), high / len(cuts))
        gain = gain * jnp.repeat(jnp.exp(steps), shape[dim] // shards_of).reshape((-1,) + (1,) * (len(shape) - 1 - dim))
    return gain


def split_up(amount, total, limit, skew):
    loads = [(1 << 20) // math.isqrt(rank ** skew) + 1 for rank in range(2, amount + 1)]
    rest, holding = total - limit - (amount - 1), [1] * (amount - 1)
    while rest > 0:
        movable = [i for i in range(amount - 1) if holding[i] < limit]
        mass, budget = sum([loads[i] for i in movable]), rest
        for i in movable:
            addition = min(limit - holding[i], max(1, budget * loads[i] // mass), rest)
            holding[i] = holding[i] + addition
            rest = rest - addition
    return np.array([limit] + holding)


def uneven(own_key, amount, total, bound, lean):
    if amount == 2:
        one = jax.random.randint(own_key, (), max(1, total - bound), min(bound, total - 1) + 1)
        return jnp.stack([one, total - one])
    tallies = jnp.asarray(split_up(amount, total, bound, lean), jnp.int32)
    couples = (amount - 1) // 2
    donor, sink = tallies[1:1 + 2 * couples:2], tallies[2:2 + 2 * couples:2]
    room = jnp.minimum(donor - 1, bound - sink)
    moved = jax.random.randint(jax.random.fold_in(own_key, 1), (couples,), 0, 1 << 20) % (room + 1)
    tallies = tallies.at[1:1 + 2 * couples:2].set(donor - moved).at[2:2 + 2 * couples:2].set(sink + moved)
    return tallies[jax.random.permutation(jax.random.fold_in(own_key, 2), amount)]


def assign_block(stream_key, own, number, rows, number_of, top, most, lean):
    ranking = jax.random.permutation(stream_key, number_of)
    heavy_load, ordinary = shares(number_of, rows * top, most, lean, True), shares(number_of, rows * top, most, lean, False)
    places = jnp.arange(number_of)

    def named(tallies, turn):
        used = int((tallies > 0).sum())
        fixed = max(1, used // 4)
        shifted = fixed + (places - fixed + turn * (used - fixed)) % max(1, number_of - fixed)
        return jnp.zeros((number_of,), jnp.int32).at[ranking[jnp.where(places < fixed, places, shifted)]].set(jnp.asarray(tallies, jnp.int32))

    tallies = jnp.where(number % 4 == 0, named(heavy_load, number // 4), named(ordinary, number - number // 4 - 1))
    mixed = jax.random.permutation(jax.random.fold_in(own, 3), number_of)
    donor, receiver = mixed[0:number_of // 2 * 2:2], mixed[1:number_of // 2 * 2:2]
    room = jnp.minimum(tallies[donor] - 1, most - tallies[receiver]) // 2
    room = jnp.where((donor == ranking[0]) | (receiver == ranking[0]) | (tallies[receiver] == 0), 0, jnp.maximum(room, 0))
    shifted = jax.random.randint(jax.random.fold_in(own, 4), (number_of // 2,), 0, 1 << 20) % (room + 1)
    tallies = tallies.at[donor].add(-shifted).at[receiver].add(shifted)
    labels = jnp.searchsorted(jnp.cumsum(tallies), jnp.arange(rows * top), side="right").astype(jnp.int32)
    listing = labels.reshape(top, rows).T
    listing = listing[jax.random.permutation(jax.random.fold_in(own, 1), rows)]
    turn = jax.random.randint(jax.random.fold_in(own, 2), (rows, 1), 0, top)
    return jnp.take_along_axis(listing, (jnp.arange(top)[None, :] + turn) % top, axis=1)


def shares(count, total, most, lean, full):
    weights = [(1 << 20) // math.isqrt(standing ** lean) + 1 for standing in range(1, count + 1)]
    largest = most if full else min(most, max(-(-total // count), total * weights[0] // sum(weights)))
    least = 1 if total - largest >= count - 1 else 0
    holding, rest = [largest] + [least] * (count - 1), total - largest - least * (count - 1)
    while rest > 0:
        candidates = [i for i in range(1, count) if holding[i] < largest] or [i for i in range(1, count) if holding[i] < most]
        pool, budget = sum([weights[i] for i in candidates]), rest
        for i in candidates:
            more = min(most - holding[i], max(1, budget * weights[i] // pool), rest)
            holding[i] = holding[i] + more
            rest = rest - more
    return np.array(holding)


def normal_values(rng, shape, width, limit, shards=(), held_as=jnp.bfloat16):
    entries = jax.random.normal(rng, shape, jnp.float32) * width
    if len(shards) > 0:
        entries = levels(rng, shape, shards, -0.22, 0.18) * entries
    return jnp.clip(entries, min=-limit, max=limit).astype(held_as)


def setup_inputs(seed: int = 0) -> dict:
    keys = jax.random.split(jax.random.key(seed), 17)
    latent = normal_values(keys[0], (TOKENS, RANK), 1.0, 6.0, ((0, 16),))
    rotary_key = draw_rotary_key(jax.random.fold_in(keys[16], 71), 0)
    doc_ids = jnp.searchsorted(jnp.cumsum(uneven(keys[2], DOCS, TOKENS, DOC_MOST, 2)), jnp.arange(TOKENS), side="right").astype(jnp.int32)
    queries_content = normal_values(keys[3], (TOKENS, HEADS * DK), 1.0, 6.0, ((0, 16), (1, 2)))
    queries_rotary = draw_queries_rotary(jax.random.fold_in(keys[16], 71), 0)
    w_key_up = normal_values(keys[5], (RANK, HEADS * DK), RANK ** -0.5, 0.375)
    w_value_up = normal_values(keys[6], (RANK, HEADS * DV), RANK ** -0.5, 0.375)
    w_out = normal_values(keys[7], (HEADS * DV, D), (HEADS * DV // 64) ** -0.5, 1.5, ((0, 2),))
    residual = normal_values(keys[8], (TOKENS, D), 0.5, 4.0, ((0, 32),))
    norm_gain = jnp.clip(1.0 + 0.18 * jax.random.normal(keys[9], (D,), jnp.float32), 0.1, 1.9)
    routes_keys = jax.random.split(jax.random.fold_in(keys[10], 1), TOKENS // ROWS)
    routes_turns = jax.random.permutation(jax.random.fold_in(keys[10], 3), TOKENS // ROWS)
    routes = jax.vmap(lambda own, number: assign_block(jax.random.fold_in(keys[10], 2), own, number, ROWS, EXPERTS, TOPK, CAP, 2))(routes_keys, routes_turns).reshape((TOKENS, TOPK))
    route_weights = jnp.clip(0.1 + 0.9 * jax.random.uniform(keys[11], (TOKENS, TOPK), jnp.float32) ** levels(keys[11], (TOKENS, TOPK), ((0, 32),), -0.2, 0.2), 0.1, 1.0)
    w_gate = normal_values(keys[12], (EXPERTS, D, FF), D ** -0.5, 0.125, ((0, 16), (2, 2)))
    w_up = normal_values(keys[13], (EXPERTS, D, FF), D ** -0.5, 0.125, ((0, 16), (2, 2)))
    w_down = normal_values(keys[14], (EXPERTS, FF, D), FF ** -0.5, 0.09375, ((0, 16), (1, 2)))
    out_gain = jnp.clip(1.0 + 0.18 * jax.random.normal(keys[15], (D,), jnp.float32), 0.1, 1.9)
    return {"latent": latent, "rotary_key": rotary_key, "doc_ids": doc_ids, "queries_content": queries_content, "queries_rotary": queries_rotary, "w_key_up": w_key_up, "w_value_up": w_value_up, "w_out": w_out, "residual": residual, "norm_gain": norm_gain, "routes": routes, "route_weights": route_weights, "w_gate": w_gate, "w_up": w_up, "w_down": w_down, "out_gain": out_gain}


ROPE_THETA = 500000.0
RESIDUAL_SCALE = 2.0 ** 0.5
NORM_EPSILON = 1e-05

def rotate(values, positions):
    half_width = values.shape[-1] // 2
    frequency = ROPE_THETA ** (-2.0 * jnp.arange(half_width, dtype=jnp.float32) / values.shape[-1])
    angles = positions.astype(jnp.float32)[:, None] * frequency[None, :]
    table_shape = (values.shape[0],) + (1,) * (values.ndim - 2) + (half_width,)
    cosine = jnp.cos(angles).reshape(table_shape)
    sine_part = jnp.sin(angles).reshape(table_shape)
    widened = values.astype(jnp.float32)
    first_half = widened[..., :half_width]
    second = widened[..., half_width:]
    return jnp.concatenate([first_half * cosine - second * sine_part, second * cosine + first_half * sine_part], -1)

def layer_norm(values, gain_vec):
    centre = lax.optimization_barrier(jnp.mean(values, -1, keepdims=True))
    spread = lax.optimization_barrier(jnp.mean(jnp.square(values - centre), -1, keepdims=True))
    return (values - centre) * lax.rsqrt(spread + NORM_EPSILON) * gain_vec

def reference(latent, rotary_key, doc_ids, queries_content, queries_rotary, w_key_up, w_value_up, w_out, residual, norm_gain, routes, route_weights, w_gate, w_up, w_down, out_gain):
    positions = jnp.arange(TOKENS, dtype=jnp.int32)
    key_content = jnp.dot(latent, w_key_up, preferred_element_type=jnp.float32).astype(jnp.bfloat16)
    key_content = key_content.reshape(TOKENS, HEADS, DK)
    values = jnp.dot(latent, w_value_up, preferred_element_type=jnp.float32).astype(jnp.bfloat16)
    values = values.reshape(TOKENS, HEADS, DV)
    key_rotary = rotate(rotary_key, positions).astype(jnp.bfloat16)
    query_rotary = rotate(queries_rotary.reshape(TOKENS, HEADS, DR), positions).astype(jnp.bfloat16)
    query_content = queries_content.reshape(TOKENS, HEADS, DK)
    padding = REACH * TOK_DEV
    key_pad = jnp.concatenate([jnp.zeros((padding, HEADS, DK), jnp.bfloat16), key_content], 0)
    value_pad = jnp.concatenate([jnp.zeros((padding, HEADS, DV), jnp.bfloat16), values], 0)
    rotary_pad = jnp.concatenate([jnp.zeros((padding, DR), jnp.bfloat16), key_rotary], 0)
    doc_pad = jnp.concatenate([jnp.full((padding,), -1, jnp.int32), doc_ids.astype(jnp.int32)], 0)
    position_pad = jnp.arange(TOKENS + padding, dtype=jnp.int32) - padding
    score_scale = (DK + DR) ** (-0.5)
    window = padding + TOK_DEV

    def attend_block(block_start):
        key_window = lax.dynamic_slice_in_dim(key_pad, block_start, window, 0).astype(jnp.float32)
        value_window = lax.dynamic_slice_in_dim(value_pad, block_start, window, 0).astype(jnp.float32)
        rotary_window = lax.dynamic_slice_in_dim(rotary_pad, block_start, window, 0).astype(jnp.float32)
        doc_window = lax.dynamic_slice_in_dim(doc_pad, block_start, window, 0)
        key_position = lax.dynamic_slice_in_dim(position_pad, block_start, window, 0)
        query_block = lax.dynamic_slice_in_dim(query_content, block_start, TOK_DEV, 0).astype(jnp.float32)
        turned_block = lax.dynamic_slice_in_dim(query_rotary, block_start, TOK_DEV, 0).astype(jnp.float32)
        query_doc = lax.dynamic_slice_in_dim(doc_ids.astype(jnp.int32), block_start, TOK_DEV, 0)
        query_position = lax.dynamic_slice_in_dim(positions, block_start, TOK_DEV, 0)
        scores = jnp.einsum('phd,qhd->hpq', query_block, key_window)
        scores = (scores + jnp.einsum('phd,qd->hpq', turned_block, rotary_window)) * score_scale
        allowed = (key_position[None, :] <= query_position[:, None]) & (key_position[None, :] >= 0)
        allowed = allowed & (doc_window[None, :] == query_doc[:, None])
        scores = jnp.where(allowed[None], scores, -jnp.inf)
        row_peak = lax.optimization_barrier(jnp.max(scores, -1, keepdims=True))
        lifted = jnp.exp(scores - row_peak)
        probability = (lifted / lax.optimization_barrier(jnp.sum(lifted, -1, keepdims=True))).astype(jnp.bfloat16)
        result = jnp.einsum('hpq,qhd->phd', probability.astype(jnp.float32), value_window)
        return result.astype(jnp.bfloat16)
    starts = jnp.arange(N_SP, dtype=jnp.int32) * TOK_DEV
    attended = lax.map(attend_block, starts).reshape(TOKENS, HEADS * DV)
    head_cols = HEADS * DV // N_TP
    projected = jnp.zeros((TOKENS, D), jnp.float32)
    for group in range(N_TP):
        partial_value = jnp.dot(attended[:, group * head_cols:(group + 1) * head_cols], w_out[group * head_cols:(group + 1) * head_cols], preferred_element_type=jnp.float32)
        projected = projected + partial_value.astype(jnp.bfloat16).astype(jnp.float32)
    normed = layer_norm(RESIDUAL_SCALE * residual.astype(jnp.float32) + projected, norm_gain).astype(jnp.bfloat16)
    capacity_all = N_SP * N_TP * CAP
    half_cols = FF // N_TP
    expert_ids = jnp.arange(EXPERTS, dtype=jnp.int32)

    def add_expert(running, inputs):
        expert_id, gate_w, up_w, down_w = inputs
        chosen = routes == expert_id
        member = jnp.any(chosen, 1)
        weight = lax.optimization_barrier(jnp.sum(jnp.where(chosen, route_weights, 0.0), 1))
        token_index = jnp.nonzero(member, size=capacity_all, fill_value=0)[0].astype(jnp.int32)
        live_mask = (jnp.arange(capacity_all) < jnp.sum(member.astype(jnp.int32))).astype(jnp.float32)
        token_rows = normed[token_index]
        gate_pre = jnp.dot(token_rows, gate_w, preferred_element_type=jnp.float32)
        upward = jnp.dot(token_rows, up_w, preferred_element_type=jnp.float32)
        hidden = (jax.nn.silu(gate_pre) * upward).astype(jnp.bfloat16)
        summed = jnp.zeros((capacity_all, D), jnp.float32)
        for group in range(N_TP):
            partial_value = jnp.dot(hidden[:, group * half_cols:(group + 1) * half_cols], down_w[group * half_cols:(group + 1) * half_cols], preferred_element_type=jnp.float32)
            summed = summed + partial_value.astype(jnp.bfloat16).astype(jnp.float32)
        expert_out = summed.astype(jnp.bfloat16).astype(jnp.float32)
        contribution = expert_out * (weight[token_index] * live_mask)[:, None]
        return (running.at[token_index].add(contribution), None)
    routed_sum, _ = lax.scan(add_expert, jnp.zeros((TOKENS, D), jnp.float32), (expert_ids, w_gate, w_up, w_down))
    combined = RESIDUAL_SCALE * normed.astype(jnp.float32) + routed_sum
    return layer_norm(combined, out_gain).astype(jnp.bfloat16)
```

```python
import functools

import jax
import jax.numpy as jnp
from jax import lax
from jax.experimental import pallas as pl
from jax.experimental.pallas import tpu as pltpu
from jax.sharding import PartitionSpec as P

HEADS = 8
DK = 128
DR = 64
DV = 128
TOPK = 2
REACH = 4
CHUNKS = 4


ROPE_THETA = 500000.0
RESIDUAL_SCALE = 2.0**0.5
NORM_EPSILON = 1e-05
MESH = pl.DeviceIdType.MESH
VMEM = pl.BlockSpec(memory_space=pltpu.VMEM)
ANY = pl.BlockSpec(memory_space=pl.ANY)
F32 = jnp.float32
BF16 = jnp.bfloat16


def rotate(values, positions):
    half_width = values.shape[-1] // 2
    frequency = ROPE_THETA ** (-2.0 * jnp.arange(half_width, dtype=jnp.float32) / values.shape[-1])
    angles = positions.astype(jnp.float32)[:, None] * frequency[None, :]
    table_shape = (values.shape[0],) + (1,) * (values.ndim - 2) + (half_width,)
    cosine = jnp.cos(angles).reshape(table_shape)
    sine_part = jnp.sin(angles).reshape(table_shape)
    widened = values.astype(jnp.float32)
    first_half = widened[..., :half_width]
    second = widened[..., half_width:]
    return jnp.concatenate(
        [first_half * cosine - second * sine_part, second * cosine + first_half * sine_part], -1
    )


def layer_norm(values, gain_vec):
    centre = jnp.mean(values, -1, keepdims=True)
    spread = jnp.mean(jnp.square(values - centre), -1, keepdims=True)
    return (values - centre) * lax.rsqrt(spread + NORM_EPSILON) * gain_vec


def dot(a, b):
    return jnp.dot(a, b, preferred_element_type=F32)


def dot_nt(a, b):
    return lax.dot_general(a, b, (((1,), (1,)), ((), ())), preferred_element_type=F32)


def remote(src, dst, send_sem, recv_sem, sp, tp):
    return pltpu.make_async_remote_copy(
        src_ref=src, dst_ref=dst, send_sem=send_sem, recv_sem=recv_sem,
        device_id=(sp, tp), device_id_type=MESH,
    )


def greet(devices):
    barrier = pltpu.get_barrier_semaphore()
    for device in devices:
        pl.semaphore_signal(barrier, inc=1, device_id=device, device_id_type=MESH)
    pl.semaphore_wait(barrier, len(devices))


def attention_kernel(
    n, pack_ref, q_ref, hot_ref, wk_ref, wv_ref, wo_ref, res_ref, gain_ref, out_ref,
    held, wo_other, scores, vals, att, att_other, send_sem, recv_sem, wo_sem, att_sem,
):
    me, tp = lax.axis_index("sp"), lax.axis_index("tp")
    tok = pack_ref.shape[0]
    rank = wk_ref.shape[0]
    heads = q_ref.shape[0]
    rows = out_ref.shape[0]
    mine = (me, tp)
    del mine
    greet(
        [(lax.rem(me + d, n), tp) for d in range(1, REACH + 1)]
        + [(lax.rem(me + n - d, n), tp) for d in range(1, REACH + 1)]
        + [(me, 1 - tp)]
    )
    copies = [None]
    for d in range(1, REACH + 1):
        copies.append(
            remote(pack_ref, held.at[d - 1], send_sem.at[d - 1], recv_sem.at[d - 1],
                   lax.rem(me + d, n), tp)
        )
        copies[d].start()
    share = remote(wo_ref, wo_other, wo_sem.at[0], wo_sem.at[1], me, 1 - tp)
    share.start()
    key_cols = pl.ds(pl.multiple_of(tp * heads * DK, 128), heads * DK)
    value_cols = pl.ds(pl.multiple_of(tp * heads * DV, 128), heads * DV)
    wk = wk_ref[:, key_cols]
    wv = wv_ref[:, value_cols]
    hot = hot_ref[...]
    for d in range(REACH + 1):
        if d == 0:
            block = pack_ref[...]
        else:
            copies[d].wait_recv()
            block = held[d - 1]
        span = slice((REACH - d) * tok, (REACH - d + 1) * tok)
        lat, tail = block[:, :rank], block[:, rank:]
        kc = dot(lat, wk).astype(BF16)
        vals[span, :] = dot(lat, wv).astype(BF16)
        allowed = dot_nt(hot, tail) > 0.5
        q_at = lax.broadcasted_iota(jnp.int32, (tok, tok), 0)
        k_at = lax.broadcasted_iota(jnp.int32, (tok, tok), 1) - d * tok
        allowed = allowed & (k_at <= q_at) & (k_at + me * tok >= 0)
        for h in range(heads):
            key = jnp.concatenate([kc[:, h * DK:(h + 1) * DK], tail], 1)
            s = dot_nt(q_ref[h], key) * ((DK + DR) ** (-0.5))
            scores[h, :, span] = jnp.where(allowed, s, -jnp.inf)
    for h in range(heads):
        s = scores[h]
        lifted = jnp.exp(s - jnp.max(s, -1, keepdims=True))
        prob = (lifted * (1.0 / jnp.sum(lifted, -1, keepdims=True))).astype(BF16)
        att[:, h * DV:(h + 1) * DV] = dot(prob, vals[:, h * DV:(h + 1) * DV]).astype(BF16)
    theirs = pl.ds(pl.multiple_of((1 - tp) * rows, rows), rows)
    ours = pl.ds(pl.multiple_of(tp * rows, rows), rows)
    swap = remote(att.at[theirs], att_other, att_sem.at[0], att_sem.at[1], me, 1 - tp)
    swap.start()
    projected = dot(att[ours, :], wo_ref[...]).astype(BF16).astype(F32)
    share.wait_recv()
    swap.wait_recv()
    projected = projected + dot(att_other[...], wo_other[...]).astype(BF16).astype(F32)
    total = RESIDUAL_SCALE * res_ref[...].astype(F32) + projected
    out_ref[...] = layer_norm(total, gain_ref[...]).astype(BF16)
    for d in range(1, REACH + 1):
        copies[d].wait_send()
    share.wait_send()
    swap.wait_send()


def attention(n, pack, q, hot, wk, wv, wo, res, gain):
    tok, wide = pack.shape
    heads = q.shape[0]
    rows, width = res.shape
    return pl.pallas_call(
        functools.partial(attention_kernel, n),
        out_shape=jax.ShapeDtypeStruct((rows, width), BF16),
        in_specs=[VMEM] * 8,
        out_specs=VMEM,
        scratch_shapes=[
            pltpu.VMEM((REACH, tok, wide), BF16),
            pltpu.VMEM(wo.shape, BF16),
            pltpu.VMEM((heads, tok, (REACH + 1) * tok), F32),
            pltpu.VMEM(((REACH + 1) * tok, heads * DV), BF16),
            pltpu.VMEM((tok, heads * DV), BF16),
            pltpu.VMEM((rows, heads * DV), BF16),
            pltpu.SemaphoreType.DMA((REACH,)),
            pltpu.SemaphoreType.DMA((REACH,)),
            pltpu.SemaphoreType.DMA((2,)),
            pltpu.SemaphoreType.DMA((2,)),
        ],
        compiler_params=pltpu.CompilerParams(
            collective_id=0, has_side_effects=True, vmem_limit_bytes=40 * 2**20
        ),
        name="attention",
    )(pack, q, hot, wk, wv, wo, res, gain)


def expert_kernel(
    n, cap, normed_ref, placing_ref, pick_ref, weight_ref, gain_ref, wg_hbm, wu_hbm, wd_hbm, out_ref,
    wg, wu, wd, outb, xin, hid, part, recvp, result, returned, total,
    w_sem, send_sem, recv_sem, fsend_sem, frecv_sem, psend_sem, precv_sem, rsend_sem, rrecv_sem,
):
    me, tp = lax.axis_index("sp"), lax.axis_index("tp")
    width = normed_ref.shape[1]
    hidden = hid.shape[1]
    per = n // CHUNKS
    tall = per * 2 * cap
    loads = [
        pltpu.make_async_copy(src, dst, w_sem.at[i])
        for i, (src, dst) in enumerate(((wg_hbm, wg), (wu_hbm, wu), (wd_hbm, wd)))
    ]
    for load in loads:
        load.start()
    normed = normed_ref[...]
    for c in range(CHUNKS):
        lines = slice(c * per * cap, (c + 1) * per * cap)
        outb[c * per:(c + 1) * per] = (
            dot(placing_ref[lines, :], normed).astype(BF16).reshape(per, cap, width)
        )
    greet([(lax.rem(me + d, n), tp) for d in range(1, n)] + [(me, 1 - tp)])
    sends, forwards, parts, returns = [None], [], [], [None]
    for d in range(1, n):
        to = lax.rem(me + d, n)
        sends.append(remote(outb.at[to], xin.at[d, tp], send_sem.at[d], recv_sem.at[d], to, tp))
        sends[d].start()
    xin[0, tp] = outb[me]
    for d in range(n):
        forwards.append(
            remote(xin.at[d, tp], xin.at[d, tp], fsend_sem.at[d], frecv_sem.at[d], me, 1 - tp)
        )
    for c in range(CHUNKS):
        group = pl.ds(c * per, per)
        parts.append(
            remote(part.at[1 - tp, group], recvp.at[group], psend_sem.at[c], precv_sem.at[c],
                   me, 1 - tp)
        )
    for d in range(1, n):
        back = lax.rem(me + n - d, n)
        returns.append(
            remote(result.at[d], returned.at[me], rsend_sem.at[d], rrecv_sem.at[d], back, tp)
        )

    def finish(c):
        parts[c].wait_recv()
        for d in range(c * per, (c + 1) * per):
            value = (part[tp, d].astype(F32) + recvp[d].astype(F32)).astype(BF16)
            if d == 0:
                returned[me] = value
            else:
                result[d] = value
                returns[d].start()

    step = 256 if hidden % 256 == 0 else 128
    for c in range(CHUNKS):
        group = range(c * per, (c + 1) * per)
        for d in group:
            if d > 0:
                sends[d].wait_recv()
            forwards[d].start()
        if c == 0:
            loads[0].wait()
            loads[1].wait()
        for d in group:
            forwards[d].wait_recv()

        def up(j, carry):
            cols = pl.ds(pl.multiple_of(j * step, step), step)
            x = xin[c * per:(c + 1) * per].reshape(tall, width)
            gate_pre = dot(x, wg[:, cols])
            upward = dot(x, wu[:, cols])
            hid[:, cols] = (gate_pre / (1.0 + jnp.exp(-gate_pre)) * upward).astype(BF16)
            return carry

        lax.fori_loop(0, hidden // step, up, 0)
        if c > 0:
            finish(c - 1)
        if c == 0:
            loads[2].wait()

        def down(j, carry):
            cols = pl.ds(pl.multiple_of(j * 512, 512), 512)
            o = dot(hid[...], wd[:, cols]).astype(BF16).reshape(per, 2, cap, 512)
            for t in range(2):
                part[t, c * per:(c + 1) * per, :, cols] = o[:, t]
            return carry

        lax.fori_loop(0, width // 512, down, 0)
        parts[c].start()
    finish(CHUNKS - 1)
    for d in range(1, n):
        returns[d].wait_recv()
    weights = weight_ref[...]
    for j in range(width // 512):
        cols = slice(j * 512, (j + 1) * 512)
        rows_back = returned[:, :, cols].reshape(n * cap, 512)
        value = RESIDUAL_SCALE * normed_ref[:, cols].astype(F32)
        for k in range(TOPK):
            value = value + weights[:, k:k + 1] * dot(pick_ref[k], rows_back)
        total[:, cols] = value
    out_ref[...] = layer_norm(total[...], gain_ref[...]).astype(BF16)
    for d in range(n):
        forwards[d].wait_send()
        if d > 0:
            sends[d].wait_send()
            returns[d].wait_send()
    for c in range(CHUNKS):
        parts[c].wait_send()


def experts(n, cap, normed, placing, pick, weights, gain, wg, wu, wd):
    rows, width = normed.shape
    hidden = wg.shape[1]
    tall = n // CHUNKS * 2 * cap
    block = (n, cap, width)
    return pl.pallas_call(
        functools.partial(expert_kernel, n, cap),
        out_shape=jax.ShapeDtypeStruct((rows, width), BF16),
        in_specs=[VMEM] * 5 + [ANY] * 3,
        out_specs=VMEM,
        scratch_shapes=[
            pltpu.VMEM(wg.shape, BF16),
            pltpu.VMEM(wu.shape, BF16),
            pltpu.VMEM(wd.shape, BF16),
            pltpu.VMEM(block, BF16),
            pltpu.VMEM((n, 2, cap, width), BF16),
            pltpu.VMEM((tall, hidden), BF16),
            pltpu.VMEM((2,) + block, BF16),
            pltpu.VMEM(block, BF16),
            pltpu.VMEM(block, BF16),
            pltpu.VMEM(block, BF16),
            pltpu.VMEM((rows, width), F32),
            pltpu.SemaphoreType.DMA((3,)),
            pltpu.SemaphoreType.DMA((n,)),
            pltpu.SemaphoreType.DMA((n,)),
            pltpu.SemaphoreType.DMA((n,)),
            pltpu.SemaphoreType.DMA((n,)),
            pltpu.SemaphoreType.DMA((CHUNKS,)),
            pltpu.SemaphoreType.DMA((CHUNKS,)),
            pltpu.SemaphoreType.DMA((n,)),
            pltpu.SemaphoreType.DMA((n,)),
        ],
        compiler_params=pltpu.CompilerParams(
            collective_id=1, has_side_effects=True, vmem_limit_bytes=58 * 2**20
        ),
        name="experts",
    )(normed, placing, pick, weights, gain, wg, wu, wd)


def per_device(
    latent,
    rotary_key,
    doc_ids,
    queries_content,
    queries_rotary,
    w_key_up,
    w_value_up,
    w_out,
    residual,
    norm_gain,
    routes,
    route_weights,
    w_gate,
    w_up,
    w_down,
    out_gain,
):
    tok_dev = latent.shape[0]
    core_count = lax.axis_size("tp")
    chip_count = lax.axis_size("sp")
    heads_here = HEADS // core_count
    sp_index = lax.axis_index("sp")
    own_position = sp_index * tok_dev + jnp.arange(tok_dev, dtype=jnp.int32)
    query_turned = rotate(queries_rotary.reshape(tok_dev, heads_here, DR), own_position).astype(BF16)
    query_block = queries_content.reshape(tok_dev, heads_here, DK)
    q = jnp.concatenate([query_block, query_turned, jnp.zeros_like(query_turned)], -1)
    q = q.transpose(1, 0, 2)
    key_turned = rotate(rotary_key, own_position).astype(BF16)
    hot = (doc_ids[:, None] == jnp.arange(DR, dtype=jnp.int32)[None, :]).astype(BF16)
    pack = jnp.concatenate([latent, key_turned, hot], 1)
    hot = jnp.concatenate([jnp.zeros_like(hot), hot], 1)
    normed = attention(
        chip_count, pack, q, hot, w_key_up, w_value_up, w_out, residual, norm_gain[None]
    )
    row_count = normed.shape[0]
    capacity = max(2, 2 * row_count * TOPK // chip_count)
    flat_route = routes.reshape(-1)
    member = (flat_route[:, None] == jnp.arange(chip_count, dtype=jnp.int32)[None, :]).astype(
        jnp.int32
    )
    slot_rank = jnp.sum((jnp.cumsum(member, 0) - member) * member, 1)
    slot_index = (flat_route * capacity + slot_rank).reshape(row_count, TOPK)
    slots = jnp.arange(chip_count * capacity, dtype=jnp.int32)
    pick = (slot_index.T[:, :, None] == slots).astype(BF16)
    placing = jnp.any(slot_index[None] == slots[:, None, None], -1).astype(BF16)
    return experts(
        chip_count, capacity, normed, placing, pick, route_weights, out_gain[None],
        w_gate[0], w_up[0], w_down[0],
    )


def solution(mesh):
    return jax.shard_map(
        per_device,
        mesh=mesh,
        in_specs=(
            P("sp", None),
            P("sp", None),
            P("sp"),
            P("sp", "tp"),
            P("sp", "tp"),
            P(),
            P(),
            P("tp", None),
            P(("sp", "tp"), None),
            P(),
            P(("sp", "tp"), None),
            P(("sp", "tp"), None),
            P("sp", None, "tp"),
            P("sp", None, "tp"),
            P("sp", "tp", None),
            P(),
        ),
        out_specs=P(("sp", "tp"), None),
        check_vma=False,
    )
```

```python
import functools

import jax
import jax.numpy as jnp
from jax import lax
from jax.experimental import pallas as pl
from jax.experimental.pallas import tpu as pltpu
from jax.sharding import PartitionSpec as P

DK = 128
DR = 64
DV = 128
TOPK = 2
REACH = 4
CHUNKS = 4


ROPE_THETA = 500000.0
RESIDUAL_SCALE = 2.0**0.5
NORM_EPSILON = 1e-05
MESH = pl.DeviceIdType.MESH
VMEM = pl.BlockSpec(memory_space=pltpu.VMEM)
ANY = pl.BlockSpec(memory_space=pl.ANY)
F32 = jnp.float32
BF16 = jnp.bfloat16


def layer_norm(values, gain_vec):
    centre = jnp.mean(values, -1, keepdims=True)
    spread = jnp.mean(jnp.square(values - centre), -1, keepdims=True)
    return (values - centre) * lax.rsqrt(spread + NORM_EPSILON) * gain_vec


def dot(a, b):
    return jnp.dot(a, b, preferred_element_type=F32)


def dot_nt(a, b):
    return lax.dot_general(a, b, (((1,), (1,)), ((), ())), preferred_element_type=F32)


def remote(src, dst, send_sem, recv_sem, sp, tp):
    return pltpu.make_async_remote_copy(
        src_ref=src, dst_ref=dst, send_sem=send_sem, recv_sem=recv_sem,
        device_id=(sp, tp), device_id_type=MESH,
    )


def flip(me, d):
    out, bit = me, 1
    while bit <= d:
        if d & bit:
            out = out + bit * (1 - 2 * (me // bit % 2))
        bit *= 2
    return out


def greet(devices):
    barrier = pltpu.get_barrier_semaphore()
    for device in devices:
        pl.semaphore_signal(barrier, inc=1, device_id=device, device_id_type=MESH)
    pl.semaphore_wait(barrier, len(devices))


def attention_kernel(
    n, lat_ref, tail_ref, qc_ref, qr_ref, cos_ref, sin_ref, wk_ref, wv_ref, wo_ref, res_ref, gain_ref,
    out_ref, held, held_tail, wo_other, scores, vals, att, att_other, send_sem, recv_sem, tsend_sem, trecv_sem, wo_sem, att_sem,
):
    me, tp = lax.axis_index("sp"), lax.axis_index("tp")
    tok = lat_ref.shape[0]
    heads = qc_ref.shape[1] // DK
    rows = out_ref.shape[0]
    greet(
        [(lax.rem(me + d, n), tp) for d in range(1, REACH + 1)]
        + [(lax.rem(me + n - d, n), tp) for d in range(1, REACH + 1)]
        + [(me, 1 - tp)]
    )
    copies, tails = [None], [None]
    for d in range(1, REACH + 1):
        to = lax.rem(me + d, n)
        copies.append(
            remote(lat_ref, held.at[d - 1], send_sem.at[d - 1], recv_sem.at[d - 1], to, tp)
        )
        tails.append(
            remote(tail_ref, held_tail.at[d - 1], tsend_sem.at[d - 1], trecv_sem.at[d - 1], to, tp)
        )
        copies[d].start()
        tails[d].start()
    share = remote(wo_ref, wo_other, wo_sem.at[0], wo_sem.at[1], me, 1 - tp)
    share.start()
    key_cols = pl.ds(pl.multiple_of(tp * heads * DK, 128), heads * DK)
    value_cols = pl.ds(pl.multiple_of(tp * heads * DV, 128), heads * DV)
    wk = wk_ref[:, key_cols]
    wv = wv_ref[:, value_cols]
    own_tail = tail_ref[...]
    tail_lane = lax.broadcasted_iota(jnp.int32, own_tail.shape, 1)
    hot = jnp.where(tail_lane >= DR, own_tail.astype(F32), 0.0).astype(BF16)
    turned = qr_ref[...]
    lanes = turned.shape[1]
    at = lax.broadcasted_iota(jnp.int32, (lanes, lanes), 1)
    source = lax.broadcasted_iota(jnp.int32, (lanes, lanes), 0)
    low = lax.rem(at, DR) < DR // 2
    partner = jnp.where(low, at + DR // 2, at - DR // 2)
    swap_mat = jnp.where(source == partner, jnp.where(low, -1.0, 1.0), 0.0).astype(BF16)
    copies_of = lanes // cos_ref.shape[1]
    cosine = jnp.concatenate([cos_ref[...]] * copies_of, 1)
    sine = jnp.concatenate([sin_ref[...]] * copies_of, 1)
    turned = (turned.astype(F32) * cosine + dot(turned, swap_mat) * sine).astype(BF16)
    wide_at = lax.broadcasted_iota(jnp.int32, (lanes, heads * 128), 1)
    wide_source = lax.broadcasted_iota(jnp.int32, (lanes, heads * 128), 0)
    spot = wide_source // DR * 128 + lax.rem(wide_source, DR)
    spread = jnp.where(wide_at == spot, 1.0, 0.0).astype(BF16)
    wide_q = dot(turned, spread).astype(BF16)
    queries = [
        jnp.concatenate([qc_ref[:, h * DK:(h + 1) * DK], wide_q[:, h * 128:(h + 1) * 128]], 1)
        for h in range(heads)
    ]
    for d in range(REACH + 1):
        if d == 0:
            lat, tail = lat_ref[...], own_tail
        else:
            copies[d].wait_recv()
            tails[d].wait_recv()
            lat, tail = held[d - 1], held_tail[d - 1]
        span = slice((REACH - d) * tok, (REACH - d + 1) * tok)
        kc = dot(lat, wk).astype(BF16)
        vals[span, :] = dot(lat, wv).astype(BF16)
        allowed = dot_nt(hot, tail) > 0.5
        q_at = lax.broadcasted_iota(jnp.int32, (tok, tok), 0)
        k_at = lax.broadcasted_iota(jnp.int32, (tok, tok), 1) - d * tok
        allowed = allowed & (k_at <= q_at) & (k_at + me * tok >= 0)
        for h in range(heads):
            key = jnp.concatenate([kc[:, h * DK:(h + 1) * DK], tail], 1)
            s = dot_nt(queries[h], key) * ((DK + DR) ** (-0.5))
            scores[h, :, span] = jnp.where(allowed, s, -jnp.inf)
    for h in range(heads):
        s = scores[h]
        lifted = jnp.exp(s - jnp.max(s, -1, keepdims=True))
        prob = (lifted * (1.0 / jnp.sum(lifted, -1, keepdims=True))).astype(BF16)
        att[:, h * DV:(h + 1) * DV] = dot(prob, vals[:, h * DV:(h + 1) * DV]).astype(BF16)
    theirs = pl.ds(pl.multiple_of((1 - tp) * rows, rows), rows)
    ours = pl.ds(pl.multiple_of(tp * rows, rows), rows)
    swap = remote(att.at[theirs], att_other, att_sem.at[0], att_sem.at[1], me, 1 - tp)
    swap.start()
    projected = dot(att[ours, :], wo_ref[...]).astype(BF16).astype(F32)
    share.wait_recv()
    swap.wait_recv()
    projected = projected + dot(att_other[...], wo_other[...]).astype(BF16).astype(F32)
    total = RESIDUAL_SCALE * res_ref[...].astype(F32) + projected
    out_ref[...] = layer_norm(total, gain_ref[...]).astype(BF16)
    for d in range(1, REACH + 1):
        copies[d].wait_send()
        tails[d].wait_send()
    share.wait_send()
    swap.wait_send()


def attention(n, latent, tail, qc, qr, cosine, sine, wk, wv, wo, res, gain):
    tok = latent.shape[0]
    heads = qc.shape[1] // DK
    rows, width = res.shape
    return pl.pallas_call(
        functools.partial(attention_kernel, n),
        out_shape=jax.ShapeDtypeStruct((rows, width), BF16),
        in_specs=[VMEM] * 11,
        out_specs=VMEM,
        scratch_shapes=[
            pltpu.VMEM((REACH,) + latent.shape, BF16),
            pltpu.VMEM((REACH,) + tail.shape, BF16),
            pltpu.VMEM(wo.shape, BF16),
            pltpu.VMEM((heads, tok, (REACH + 1) * tok), F32),
            pltpu.VMEM(((REACH + 1) * tok, heads * DV), BF16),
            pltpu.VMEM((tok, heads * DV), BF16),
            pltpu.VMEM((rows, heads * DV), BF16),
            pltpu.SemaphoreType.DMA((REACH,)),
            pltpu.SemaphoreType.DMA((REACH,)),
            pltpu.SemaphoreType.DMA((REACH,)),
            pltpu.SemaphoreType.DMA((REACH,)),
            pltpu.SemaphoreType.DMA((2,)),
            pltpu.SemaphoreType.DMA((2,)),
        ],
        compiler_params=pltpu.CompilerParams(
            collective_id=0, has_side_effects=True, vmem_limit_bytes=40 * 2**20
        ),
        name="attention",
    )(latent, tail, qc, qr, cosine, sine, wk, wv, wo, res, gain)


def expert_kernel(
    n, cap, normed_ref, slot_ref, slot_row_ref, weight_ref, gain_ref, wg_hbm, wu_hbm, wd_hbm, out_ref,
    wg, wu, wd, outb, xin, hid, part, recvp, result, returned, total,
    w_sem, send_sem, recv_sem, fsend_sem, frecv_sem, psend_sem, precv_sem, rsend_sem, rrecv_sem,
):
    me, tp = lax.axis_index("sp"), lax.axis_index("tp")
    rows, width = normed_ref.shape
    hidden = hid.shape[1]
    per = n // CHUNKS
    tall = per * 2 * cap
    loads = [
        pltpu.make_async_copy(src, dst, w_sem.at[i])
        for i, (src, dst) in enumerate(((wg_hbm, wg), (wu_hbm, wu), (wd_hbm, wd)))
    ]
    for load in loads:
        load.start()
    normed = normed_ref[...]
    for c in range(CHUNKS):
        line = lax.broadcasted_iota(jnp.int32, (per * cap, rows), 0) + c * per * cap
        placing = jnp.zeros(line.shape, F32)
        for k in range(TOPK):
            placing = jnp.where(line == slot_row_ref[k:k + 1, :], 1.0, placing)
        outb[c * per:(c + 1) * per] = (
            dot(placing.astype(BF16), normed).astype(BF16).reshape(per, cap, width)
        )
    greet([(lax.rem(me + d, n), tp) for d in range(1, n)] + [(me, 1 - tp)])
    sends, forwards, parts, returns = [None], [], [], [None]
    for d in range(1, n):
        to = flip(me, d)
        sends.append(remote(outb.at[to], xin.at[d, tp], send_sem.at[d], recv_sem.at[d], to, tp))
        sends[d].start()
    xin[0, tp] = outb[me]
    for d in range(n):
        forwards.append(
            remote(xin.at[d, tp], xin.at[d, tp], fsend_sem.at[d], frecv_sem.at[d], me, 1 - tp)
        )
    for c in range(CHUNKS):
        group = pl.ds(c * per, per)
        parts.append(
            remote(part.at[1 - tp, group], recvp.at[group], psend_sem.at[c], precv_sem.at[c],
                   me, 1 - tp)
        )
    for d in range(1, n):
        back = flip(me, d)
        returns.append(
            remote(result.at[d], returned.at[me], rsend_sem.at[d], rrecv_sem.at[d], back, tp)
        )

    def finish(c):
        parts[c].wait_recv()
        for d in range(c * per, (c + 1) * per):
            value = (part[tp, d].astype(F32) + recvp[d].astype(F32)).astype(BF16)
            if d == 0:
                returned[me] = value
            else:
                result[d] = value
                returns[d].start()

    step = 256 if hidden % 256 == 0 else 128
    for c in range(CHUNKS):
        group = range(c * per, (c + 1) * per)
        for d in group:
            if d > 0:
                sends[d].wait_recv()
            forwards[d].start()
        if c == 0:
            loads[0].wait()
            loads[1].wait()
        for d in group:
            forwards[d].wait_recv()

        def up(j, carry):
            cols = pl.ds(pl.multiple_of(j * step, step), step)
            x = xin[c * per:(c + 1) * per].reshape(tall, width)
            gate_pre = dot(x, wg[:, cols])
            upward = dot(x, wu[:, cols])
            hid[:, cols] = (gate_pre / (1.0 + jnp.exp(-gate_pre)) * upward).astype(BF16)
            return carry

        lax.fori_loop(0, hidden // step, up, 0)
        if c > 0:
            finish(c - 1)
        if c == 0:
            loads[2].wait()

        def down(j, carry):
            cols = pl.ds(pl.multiple_of(j * 512, 512), 512)
            o = dot(hid[...], wd[:, cols]).astype(BF16).reshape(per, 2, cap, 512)
            for t in range(2):
                part[t, c * per:(c + 1) * per, :, cols] = o[:, t]
            return carry

        lax.fori_loop(0, width // 512, down, 0)
        parts[c].start()
    finish(CHUNKS - 1)
    for d in range(1, n):
        returns[d].wait_recv()
    weights = weight_ref[...]
    slot_at = lax.broadcasted_iota(jnp.int32, (rows, n * cap), 1)
    picks = [
        jnp.where(slot_at == slot_ref[:, k:k + 1], 1.0, 0.0).astype(BF16) for k in range(TOPK)
    ]
    for j in range(width // 512):
        cols = slice(j * 512, (j + 1) * 512)
        rows_back = returned[:, :, cols].reshape(n * cap, 512)
        value = RESIDUAL_SCALE * normed_ref[:, cols].astype(F32)
        for k in range(TOPK):
            value = value + weights[:, k:k + 1] * dot(picks[k], rows_back)
        total[:, cols] = value
    out_ref[...] = layer_norm(total[...], gain_ref[...]).astype(BF16)
    for d in range(n):
        forwards[d].wait_send()
        if d > 0:
            sends[d].wait_send()
            returns[d].wait_send()
    for c in range(CHUNKS):
        parts[c].wait_send()


def experts(n, cap, normed, slots, slot_rows, weights, gain, wg, wu, wd):
    rows, width = normed.shape
    hidden = wg.shape[1]
    tall = n // CHUNKS * 2 * cap
    block = (n, cap, width)
    return pl.pallas_call(
        functools.partial(expert_kernel, n, cap),
        out_shape=jax.ShapeDtypeStruct((rows, width), BF16),
        in_specs=[VMEM] * 5 + [ANY] * 3,
        out_specs=VMEM,
        scratch_shapes=[
            pltpu.VMEM(wg.shape, BF16),
            pltpu.VMEM(wu.shape, BF16),
            pltpu.VMEM(wd.shape, BF16),
            pltpu.VMEM(block, BF16),
            pltpu.VMEM((n, 2, cap, width), BF16),
            pltpu.VMEM((tall, hidden), BF16),
            pltpu.VMEM((2,) + block, BF16),
            pltpu.VMEM(block, BF16),
            pltpu.VMEM(block, BF16),
            pltpu.VMEM(block, BF16),
            pltpu.VMEM((rows, width), F32),
            pltpu.SemaphoreType.DMA((3,)),
            pltpu.SemaphoreType.DMA((n,)),
            pltpu.SemaphoreType.DMA((n,)),
            pltpu.SemaphoreType.DMA((n,)),
            pltpu.SemaphoreType.DMA((n,)),
            pltpu.SemaphoreType.DMA((CHUNKS,)),
            pltpu.SemaphoreType.DMA((CHUNKS,)),
            pltpu.SemaphoreType.DMA((n,)),
            pltpu.SemaphoreType.DMA((n,)),
        ],
        compiler_params=pltpu.CompilerParams(
            collective_id=1, has_side_effects=True, vmem_limit_bytes=58 * 2**20
        ),
        name="experts",
    )(normed, slots, slot_rows, weights, gain, wg, wu, wd)


def per_device(
    latent,
    rotary_key,
    doc_ids,
    queries_content,
    queries_rotary,
    w_key_up,
    w_value_up,
    w_out,
    residual,
    norm_gain,
    routes,
    route_weights,
    w_gate,
    w_up,
    w_down,
    out_gain,
):
    tok_dev = latent.shape[0]
    chip_count = lax.axis_size("sp")
    sp_index = lax.axis_index("sp")
    own_position = sp_index * tok_dev + jnp.arange(tok_dev, dtype=jnp.int32)
    lane = jnp.arange(128, dtype=jnp.int32) % (DR // 2)
    frequency = ROPE_THETA ** (-2.0 * lane.astype(F32) / DR)
    angles = own_position.astype(F32)[:, None] * frequency[None, :]
    cosine, sine = jnp.cos(angles), jnp.sin(angles)
    half = DR // 2
    first, second = rotary_key[:, :half].astype(F32), rotary_key[:, half:].astype(F32)
    cos_half, sin_half = cosine[:, :half], sine[:, :half]
    hot = (doc_ids[:, None] == jnp.arange(DR, dtype=jnp.int32)[None, :]).astype(BF16)
    tail = jnp.concatenate(
        [
            (first * cos_half - second * sin_half).astype(BF16),
            (second * cos_half + first * sin_half).astype(BF16),
            hot,
        ],
        1,
    )
    normed = attention(
        chip_count, latent, tail, queries_content, queries_rotary, cosine, sine,
        w_key_up, w_value_up, w_out, residual, norm_gain[None],
    )
    row_count = normed.shape[0]
    capacity = max(2, 2 * row_count * TOPK // chip_count)
    flat_route = routes.reshape(-1)
    member = (flat_route[:, None] == jnp.arange(chip_count, dtype=jnp.int32)[None, :]).astype(
        jnp.int32
    )
    slot_rank = jnp.sum((jnp.cumsum(member, 0) - member) * member, 1)
    slot_index = (flat_route * capacity + slot_rank).reshape(row_count, TOPK)
    return experts(
        chip_count, capacity, normed, slot_index, slot_index.T, route_weights, out_gain[None],
        w_gate[0], w_up[0], w_down[0],
    )


def solution(mesh):
    return jax.shard_map(
        per_device,
        mesh=mesh,
        in_specs=(
            P("sp", None),
            P("sp", None),
            P("sp"),
            P("sp", "tp"),
            P("sp", "tp"),
            P(),
            P(),
            P("tp", None),
            P(("sp", "tp"), None),
            P(),
            P(("sp", "tp"), None),
            P(("sp", "tp"), None),
            P("sp", None, "tp"),
            P("sp", None, "tp"),
            P("sp", "tp", None),
            P(),
        ),
        out_specs=P(("sp", "tp"), None),
        check_vma=False,
    )
```
